32 devices in a mesh: sp: 8 (over z, y), tp: 4 (over x, core).
Axes of the slice: x: 2, y: 2, z: 4, core: 2. Of those that a mesh axis runs over, the one named last changes fastest.
Arguments:
- tokens_in: bfloat16 [2048, 2048], P('sp'), may hold values from -3 to 3
- queries: bfloat16 [2048, 1024], P('sp', 'tp'), may hold values from -6 to 6
- keys: bfloat16 [2048, 256], P('sp', 'tp'), may hold values from -6 to 6
- values: bfloat16 [2048, 256], P('sp', 'tp'), may hold values from -12 to 12
- doc_ids: int32 [2048], P('sp'), may hold values from 0 to 1, never falling along the last dimension, each value on 1 to 1280 neighbouring positions
- query_gain: float32 [64], replicated, may hold values from 2.5 to 6
- key_norm_scale: float32 [64], replicated, may hold values from 2.5 to 6
- out_weight: bfloat16 [1024, 2048], P('tp'), may hold values from -0.1875 to 0.1875
- norm_gain: float32 [2048], replicated, may hold values from 0.1 to 1.9
- gate_weight: bfloat16 [2048, 5632], P('sp', 'tp'), may hold values from -0.125 to 0.125
- up_weight: bfloat16 [2048, 5632], P('sp', 'tp'), may hold values from -0.125 to 0.125
- down_weight: bfloat16 [5632, 2048], P('tp', 'sp'), may hold values from -0.078125 to 0.078125
Outputs:
- layer_out: bfloat16 [2048, 2048], P('sp')
The draws below stay inside these ranges and needn't reach their ends.
Inputs may be any that keep to these rules, and one draw needn't show every extreme that they name: `doc_ids`: document numbers never fall along the sequence; every document has 1 to 1280 positions and one has exactly 1280.
All inputs are finite; a program needn't handle non-finite values.
Results may differ from the reference program's by a relative error of at most 0.014.
The reference program's roundings to bfloat16 on the way (of `weights`, `attended`, `normed` and `hidden`) count: a program that leaves them out, or rounds other values in their place, can miss the bound.
Values may be sent and summed in bfloat16 or wider, within the bound.
A program may use at most 128 MiB of HBM per device.

```python
import math
import jax
import jax.numpy as jnp
import numpy as np
from jax import lax

D = 2048
QUERY_HEADS = 16
KEY_VALUE_HEADS = 4
HEAD_SIZE = 64
FF = 5632
GRID = 64
PACKED_TOKENS = 2048
DOCS = 2
DOC_MOST = 1280
N_TP = 4


def repeated_keys(key):
    sampled_values = jax.random.normal(jax.random.fold_in(key, 11), (PACKED_TOKENS, KEY_VALUE_HEADS * HEAD_SIZE), jnp.float32)
    return jnp.clip(sampled_values, -6.0, 6.0)


def draw_keys(key, part):
    return repeated_keys(key).astype(jnp.bfloat16)


def draw_queries(key, part):
    fresh = jnp.clip(jax.random.normal(jax.random.fold_in(key, 12), (PACKED_TOKENS, QUERY_HEADS * HEAD_SIZE), jnp.float32), -6.0, 6.0)
    return fresh.astype(jnp.bfloat16)


def draw_query_gain(key, part):
    spread = jax.random.uniform(jax.random.fold_in(key, 21), (HEAD_SIZE,), jnp.float32)
    return 2.5 + spread


def draw_key_norm_scale(key, part):
    spread = jax.random.uniform(jax.random.fold_in(key, 22), (HEAD_SIZE,), jnp.float32)
    return 2.5 + spread


def shard_levels(own_key, extent, shards, least, largest):
    def one(dim, parts):
        heights = jax.random.uniform(jax.random.fold_in(jax.random.fold_in(own_key, 6), dim), (parts,), jnp.float32, least / len(shards), largest / len(shards))
        return jnp.repeat(jnp.exp(heights), extent[dim] // parts).reshape((-1,) + (1,) * (len(extent) - dim - 1))

    level = one(*shards[0])
    for cut in shards[1:]:
        level = level * one(*cut)
    return level


def split_up(amount, total, bound, skew):
    loads = [(1 << 20) // math.isqrt(rank ** skew) + 1 for rank in range(2, amount + 1)]
    surplus, counts = total - bound - (amount - 1), [1] * (amount - 1)
    while surplus > 0:
        movable = [i for i in range(amount - 1) if counts[i] < bound]
        mass, remaining = sum([loads[i] for i in movable]), surplus
        for i in movable:
            more = min(bound - counts[i], max(1, remaining * loads[i] // mass), surplus)
            counts[i] = counts[i] + more
            surplus = surplus - more
    return np.array([bound] + counts)


def ragged_sizes(stream_key, amount, total, limit, lean):
    if amount == 2:
        one = jax.random.randint(stream_key, (), max(1, total - limit), min(limit, total - 1) + 1)
        return jnp.stack([one, total - one])
    lengths = jnp.asarray(split_up(amount, total, limit, lean), jnp.int32)
    couples = (amount - 1) // 2
    giver, receiver = lengths[1:1 + 2 * couples:2], lengths[2:2 + 2 * couples:2]
    margin = jnp.minimum(giver - 1, limit - receiver)
    moved = jax.random.randint(jax.random.fold_in(stream_key, 1), (couples,), 0, 1 << 20) % (margin + 1)
    lengths = lengths.at[1:1 + 2 * couples:2].set(giver - moved).at[2:2 + 2 * couples:2].set(receiver + moved)
    return lengths[jax.random.permutation(jax.random.fold_in(stream_key, 2), amount)]


def scatter_about(own_key, dims, width, bound, shards=(), kind=jnp.bfloat16):
    level = shard_levels(own_key, dims, shards, -0.22, 0.18) if shards else 1.0
    drawn = jax.random.normal(own_key, dims, jnp.float32) * width * level
    return jnp.minimum(jnp.maximum(drawn, -bound), bound).astype(kind)


def setup_inputs(seed: int = 0) -> dict:
    key_list = jax.random.split(jax.random.key(seed), 13)
    return {
        "tokens_in": scatter_about(key_list[0], (PACKED_TOKENS, D), 0.5, 3.0, ((0, 8),)),
        "queries": draw_queries(jax.random.fold_in(key_list[12], 71), 0),
        "keys": draw_keys(jax.random.fold_in(key_list[12], 71), 0),
        "values": scatter_about(key_list[3], (PACKED_TOKENS, KEY_VALUE_HEADS * HEAD_SIZE), 2.0, 12.0, ((0, 8), (1, 4))),
        "doc_ids": jnp.searchsorted(jnp.cumsum(ragged_sizes(key_list[4], DOCS, PACKED_TOKENS, DOC_MOST, 1)), jnp.arange(PACKED_TOKENS), side="right").astype(jnp.int32),
        "query_gain": draw_query_gain(jax.random.fold_in(key_list[12], 71), 0),
        "key_norm_scale": draw_key_norm_scale(jax.random.fold_in(key_list[12], 71), 0),
        "out_weight": scatter_about(key_list[7], (QUERY_HEADS * HEAD_SIZE, D), (QUERY_HEADS * HEAD_SIZE) ** -0.5, 0.1875, ((0, 4),)),
        "norm_gain": jnp.clip(1.0 + 0.18 * jax.random.normal(key_list[8], (D,), jnp.float32), 0.1, 1.9),
        "gate_weight": scatter_about(key_list[9], (D, FF), D ** -0.5, 0.125, ((0, 8), (1, 4))),
        "up_weight": scatter_about(key_list[10], (D, FF), D ** -0.5, 0.125, ((0, 8), (1, 4))),
        "down_weight": scatter_about(key_list[11], (FF, D), FF ** -0.5, 0.078125, ((0, 4), (1, 8))),
    }


EPS = 1e-06
THETA = 10000.0
NEG = -1e+30

def rotate_half(block, angle):
    half_dim = block.shape[-1] // 2
    cosine = jnp.cos(angle)[:, None, :]
    sine = jnp.sin(angle)[:, None, :]
    first = block[..., :half_dim]
    second = block[..., half_dim:]
    return jnp.concatenate([first * cosine - second * sine, second * cosine + first * sine], axis=-1)

def normalized_rotated(values_in, gain, heads, lattice_row, lattice_column):
    full = values_in.astype(jnp.float32).reshape(values_in.shape[0], heads, -1)
    full = full * lax.rsqrt(lax.optimization_barrier(jnp.mean(full * full, axis=-1, keepdims=True)) + EPS) * gain
    half_dim = full.shape[-1] // 2
    freqs = THETA ** (-2.0 * jnp.arange(half_dim // 2, dtype=jnp.float32) / half_dim)
    by_row = rotate_half(full[..., :half_dim], lattice_row[:, None] * freqs[None, :])
    by_col = rotate_half(full[..., half_dim:], lattice_column[:, None] * freqs[None, :])
    return jnp.concatenate([by_row, by_col], axis=-1).astype(jnp.bfloat16)

def reference(tokens_in, queries, keys, values, doc_ids, query_gain, key_norm_scale, out_weight, norm_gain, gate_weight, up_weight, down_weight):
    places = jnp.arange(PACKED_TOKENS, dtype=jnp.int32)
    lattice_row = (places // GRID).astype(jnp.float32)
    lattice_column = (places % GRID).astype(jnp.float32)
    q_all = normalized_rotated(queries, query_gain, QUERY_HEADS, lattice_row, lattice_column)
    every_key = normalized_rotated(keys, key_norm_scale, KEY_VALUE_HEADS, lattice_row, lattice_column).astype(jnp.float32)
    every_value = values.reshape(PACKED_TOKENS, KEY_VALUE_HEADS, HEAD_SIZE).astype(jnp.float32)
    query_group = QUERY_HEADS // KEY_VALUE_HEADS
    scale = HEAD_SIZE ** (-0.5)
    rows_per_block = 128

    def attend(start):
        query_tile = lax.dynamic_slice_in_dim(q_all, start, rows_per_block, 0).astype(jnp.float32)
        query_tile = query_tile.reshape(rows_per_block, KEY_VALUE_HEADS, query_group, HEAD_SIZE)
        doc_block = lax.dynamic_slice_in_dim(doc_ids, start, rows_per_block, 0)
        scores = jnp.einsum('qhgd,khd->hgqk', query_tile, every_key) * scale
        same = (doc_block[:, None] == doc_ids[None, :])[None, None]
        scores = jnp.where(same, scores, NEG)
        top = lax.optimization_barrier(jnp.max(scores, axis=-1, keepdims=True))
        weights = jnp.where(same, jnp.exp(scores - top), 0.0)
        total = lax.optimization_barrier(jnp.sum(weights, axis=-1))
        rounded = lax.optimization_barrier(weights.astype(jnp.bfloat16)).astype(jnp.float32)
        blended = jnp.einsum('hgqk,khd->hgqd', rounded, every_value) / total[..., None]
        return blended.transpose(2, 0, 1, 3).reshape(rows_per_block, QUERY_HEADS * HEAD_SIZE).astype(jnp.bfloat16)
    starts = jnp.arange(PACKED_TOKENS // rows_per_block, dtype=jnp.int32) * rows_per_block
    attended = lax.map(attend, starts).reshape(PACKED_TOKENS, QUERY_HEADS * HEAD_SIZE)
    share_cols = QUERY_HEADS * HEAD_SIZE // N_TP
    mixed = jnp.zeros((PACKED_TOKENS, D), jnp.float32)
    for member in range(N_TP):
        part_out = jnp.dot(attended[:, member * share_cols:(member + 1) * share_cols], out_weight[member * share_cols:(member + 1) * share_cols], preferred_element_type=jnp.float32)
        mixed = mixed + part_out.astype(jnp.bfloat16).astype(jnp.float32)
    resid = tokens_in.astype(jnp.float32) + mixed
    normed = (resid * lax.rsqrt(lax.optimization_barrier(jnp.mean(resid * resid, axis=-1, keepdims=True)) + EPS) * norm_gain).astype(jnp.bfloat16)
    gate = jnp.dot(normed, gate_weight, preferred_element_type=jnp.float32)
    up_val = jnp.dot(normed, up_weight, preferred_element_type=jnp.float32)
    hidden = (jax.nn.silu(gate) * up_val).astype(jnp.bfloat16)
    unit_cols = FF // N_TP
    fed = jnp.zeros((PACKED_TOKENS, D), jnp.float32)
    for member in range(N_TP):
        part_out = jnp.dot(hidden[:, member * unit_cols:(member + 1) * unit_cols], down_weight[member * unit_cols:(member + 1) * unit_cols], preferred_element_type=jnp.float32)
        fed = fed + part_out.astype(jnp.bfloat16).astype(jnp.float32)
    return (resid + fed).astype(jnp.bfloat16)
```

```python
import functools

import jax
import jax.numpy as jnp
from jax import lax
from jax.experimental import pallas as pl
from jax.experimental.pallas import tpu as pltpu
from jax.sharding import PartitionSpec as P

GRID = 64


EPS = 1e-06
THETA = 10000.0
NEG = -1e30


def rotate_half(block, angle):
    half_dim = block.shape[-1] // 2
    cosine = jnp.cos(angle)[:, None, :]
    sine = jnp.sin(angle)[:, None, :]
    first = block[..., :half_dim]
    second = block[..., half_dim:]
    return jnp.concatenate(
        [first * cosine - second * sine, second * cosine + first * sine], axis=-1
    )


def normalized_rotated(values_in, gain, heads, lattice_row, lattice_column):
    full = values_in.astype(jnp.float32).reshape(values_in.shape[0], heads, -1)
    full = full * lax.rsqrt(jnp.mean(full * full, axis=-1, keepdims=True) + EPS) * gain
    half_dim = full.shape[-1] // 2
    freqs = THETA ** (-2.0 * jnp.arange(half_dim // 2, dtype=jnp.float32) / half_dim)
    by_row = rotate_half(full[..., :half_dim], lattice_row[:, None] * freqs[None, :])
    by_col = rotate_half(full[..., half_dim:], lattice_column[:, None] * freqs[None, :])
    return jnp.concatenate([by_row, by_col], axis=-1).astype(jnp.bfloat16)


MESH = pl.DeviceIdType.MESH
VM = pl.BlockSpec(memory_space=pltpu.VMEM)


def params(cid):
    return pltpu.CompilerParams(
        collective_id=cid, has_side_effects=True, vmem_limit_bytes=56 * 1024 * 1024
    )


def greet(count, where):
    barrier = pltpu.get_barrier_semaphore()

    @pl.loop(1, count)
    def _(step):
        pl.semaphore_signal(barrier, inc=1, device_id=where(step), device_id_type=MESH)

    pl.semaphore_wait(barrier, count - 1)


def gather_kernel(n, kv_ref, doc_ref, kv_out, doc_out, send, recv, doc_send, doc_recv):
    me = lax.axis_index("sp")

    def where(step):
        return {"sp": lax.rem(me + step, n)}

    def copies(step, slot):
        return (
            pltpu.make_async_remote_copy(
                kv_ref, kv_out.at[slot], send.at[step], recv.at[step], where(step), MESH
            ),
            pltpu.make_async_remote_copy(
                doc_ref, doc_out.at[slot], doc_send.at[step], doc_recv.at[step], where(step), MESH
            ),
        )

    greet(n, where)

    @pl.loop(1, n)
    def _(step):
        for copy in copies(step, me):
            copy.start()

    kv_out[me] = kv_ref[...]
    doc_out[me] = doc_ref[...]

    @pl.loop(1, n)
    def _(step):
        for copy in copies(step, lax.rem(me + n - step, n)):
            copy.wait_recv()
            copy.wait_send()


def gather_sp(n, packed, docs):
    return pl.pallas_call(
        functools.partial(gather_kernel, n),
        out_shape=(
            jax.ShapeDtypeStruct((n,) + packed.shape, packed.dtype),
            jax.ShapeDtypeStruct((n,) + docs.shape, docs.dtype),
        ),
        in_specs=[VM, VM],
        out_specs=(VM, VM),
        scratch_shapes=[pltpu.SemaphoreType.DMA((n,))] * 4,
        compiler_params=params(0),
        name="gather_sp",
    )(packed, docs)


def mid_kernel(
    nt, partial_ref, tokens_ref, gain_ref, normed_out, resid_out, landing, send, recv, send2, recv2
):
    sp, tp = lax.axis_index("sp"), lax.axis_index("tp")
    side = lax.rem(sp, 2)
    base = sp - side
    group = 2 * nt
    me = side * nt + tp
    rows = resid_out.shape[0]

    def where(step):
        other = lax.rem(me + step, group)
        return {"sp": base + other // nt, "tp": lax.rem(other, nt)}

    def part(step):
        peer = lax.rem(tp + step, nt)
        return pltpu.make_async_remote_copy(
            partial_ref.at[peer],
            landing.at[step],
            send.at[step],
            recv.at[step],
            {"sp": sp, "tp": peer},
            MESH,
        )

    def spread(step, slot):
        return pltpu.make_async_remote_copy(
            normed_out.at[slot], normed_out.at[slot], send2.at[step], recv2.at[step], where(step), MESH
        )

    greet(group, where)
    for step in range(1, nt):
        part(step).start()
    for step in range(1, nt):
        part(step).wait_recv()
    chunk = 16

    @pl.loop(0, rows // chunk)
    def _(i):
        at = pl.ds(pl.multiple_of(i * chunk, chunk), chunk)
        mixed = partial_ref[tp, at].astype(jnp.float32)
        for step in range(1, nt):
            mixed = mixed + landing[step, at].astype(jnp.float32)
        resid = tokens_ref[tp, at].astype(jnp.float32) + mixed
        resid_out[at] = resid
        power = jnp.mean(resid * resid, axis=-1, keepdims=True)
        normed_out[me, at] = (resid * lax.rsqrt(power + EPS) * gain_ref[...]).astype(jnp.bfloat16)

    for step in range(1, group):
        spread(step, me).start()
    for step in range(1, group):
        copy = spread(step, lax.rem(me + group - step, group))
        copy.wait_recv()
        copy.wait_send()
    for step in range(1, nt):
        part(step).wait_send()


def mid_stage(nt, part, tokens, gain):
    rows, width = part.shape[0] // nt, part.shape[1]
    return pl.pallas_call(
        functools.partial(mid_kernel, nt),
        out_shape=(
            jax.ShapeDtypeStruct((2 * nt, rows, width), jnp.bfloat16),
            jax.ShapeDtypeStruct((rows, width), jnp.float32),
        ),
        in_specs=[VM, VM, VM],
        out_specs=(VM, VM),
        scratch_shapes=[pltpu.VMEM((nt, rows, width), jnp.bfloat16)]
        + [pltpu.SemaphoreType.DMA((nt,))] * 2
        + [pltpu.SemaphoreType.DMA((2 * nt,))] * 2,
        compiler_params=params(1),
        name="mid_stage",
    )(part.reshape(nt, rows, width), tokens.reshape(nt, rows, width), gain.reshape(1, width))


def last_kernel(nt, fed_ref, resid_ref, out_ref, landing, send, recv, send2, recv2):
    sp, tp = lax.axis_index("sp"), lax.axis_index("tp")
    side = lax.rem(sp, 2)
    base = sp - side
    group = 2 * nt
    me = side * nt + tp
    rows = resid_ref.shape[0]

    def where(step):
        other = lax.rem(me + step, group)
        return {"sp": base + other // nt, "tp": lax.rem(other, nt)}

    def part(step):
        return pltpu.make_async_remote_copy(
            fed_ref.at[lax.rem(me + step, group)],
            landing.at[step],
            send.at[step],
            recv.at[step],
            where(step),
            MESH,
        )

    def spread(step, slot):
        return pltpu.make_async_remote_copy(
            out_ref.at[slot],
            out_ref.at[slot],
            send2.at[step],
            recv2.at[step],
            {"sp": sp, "tp": lax.rem(tp + step, nt)},
            MESH,
        )

    greet(group, where)
    for step in range(1, group):
        part(step).start()
    for step in range(1, group):
        part(step).wait_recv()
    chunk = 16

    @pl.loop(0, rows // chunk)
    def _(i):
        at = pl.ds(pl.multiple_of(i * chunk, chunk), chunk)
        fed = fed_ref[me, at].astype(jnp.float32)
        for step in range(1, group):
            fed = fed + landing[step, at].astype(jnp.float32)
        out_ref[tp, at] = (resid_ref[at] + fed).astype(jnp.bfloat16)

    for step in range(1, nt):
        spread(step, tp).start()
    for step in range(1, nt):
        copy = spread(step, lax.rem(tp + nt - step, nt))
        copy.wait_recv()
        copy.wait_send()
    for step in range(1, group):
        part(step).wait_send()


def last_stage(nt, fed, resid):
    rows, width = resid.shape
    return pl.pallas_call(
        functools.partial(last_kernel, nt),
        out_shape=jax.ShapeDtypeStruct((nt, rows, width), jnp.bfloat16),
        in_specs=[VM, VM],
        out_specs=VM,
        scratch_shapes=[pltpu.VMEM((2 * nt, rows, width), jnp.bfloat16)]
        + [pltpu.SemaphoreType.DMA((2 * nt,))] * 2
        + [pltpu.SemaphoreType.DMA((nt,))] * 2,
        compiler_params=params(2),
        name="last_stage",
    )(fed.reshape(2 * nt, rows, width), resid)


def pair_share(n, arrays, axis, joins):
    side = lax.rem(lax.axis_index("sp"), 2)
    own, away = [], []
    for array in arrays:
        half = array.shape[axis] // 2
        own.append(lax.dynamic_slice_in_dim(array, side * half, half, axis))
        away.append(lax.dynamic_slice_in_dim(array, (1 - side) * half, half, axis))
    own = jnp.concatenate(own, axis=axis)
    away = jnp.concatenate(away, axis=axis)
    came = lax.ppermute(away, "sp", [(i, i ^ 1) for i in range(n)])
    first = jnp.where(side == 0, own, came)
    second = jnp.where(side == 0, came, own)
    return jnp.concatenate([first, second], axis=joins)


def per_device(
    n,
    nt,
    tokens_in,
    queries,
    keys,
    values,
    doc_ids,
    query_gain,
    key_norm_scale,
    out_weight,
    norm_gain,
    gate_weight,
    up_weight,
    down_weight,
):
    tok_rows = tokens_in.shape[0]
    head_dim = query_gain.shape[0]
    local_heads = queries.shape[1] // head_dim
    places = lax.axis_index("sp") * tok_rows + jnp.arange(tok_rows, dtype=jnp.int32)
    lattice_row = (places // GRID).astype(jnp.float32)
    lattice_column = (places % GRID).astype(jnp.float32)
    q_local = normalized_rotated(queries, query_gain, local_heads, lattice_row, lattice_column)
    q_rows = q_local.transpose(1, 0, 2).reshape(local_heads * tok_rows, head_dim)
    lanes = [[2 * j + side for j in range(n // 2)] for side in range(2)]
    gate_up_all = lax.all_gather(
        pair_share(n, [gate_weight, up_weight], 1, 0), "sp", axis_index_groups=lanes, axis=0, tiled=True
    )
    down_all = lax.all_gather(
        pair_share(n, [down_weight], 0, 1), "sp", axis_index_groups=lanes, axis=1, tiled=True
    )
    turned = normalized_rotated(keys, key_norm_scale, 1, lattice_row, lattice_column)
    packed = jnp.concatenate([turned.reshape(tok_rows, head_dim), values], axis=1)
    kv_all, doc_all = gather_sp(n, packed, doc_ids.reshape(1, tok_rows))
    row_docs = jnp.tile(doc_ids, local_heads)
    first_doc = doc_ids[0]
    last_doc = doc_ids[-1]
    scale = head_dim ** (-0.5)
    total_rows = local_heads * tok_rows

    def absorb_block(state, key_block, value_block, doc_block):

        def absorb(current):
            running_max, running_sum, running_acc = current
            scores = (
                jnp.einsum("qd,kd->qk", q_rows, key_block, preferred_element_type=jnp.float32)
                * scale
            )
            same = row_docs[:, None] == doc_block[None, :]
            scores = jnp.where(same, scores, NEG)
            new_max = jnp.maximum(running_max, jnp.max(scores, axis=1))
            weights = jnp.where(same, jnp.exp(scores - new_max[:, None]), 0.0)
            shrink = jnp.exp(running_max - new_max)
            new_sum = running_sum * shrink + jnp.sum(weights, axis=1)
            new_acc = running_acc * shrink[:, None] + jnp.dot(
                weights.astype(jnp.bfloat16), value_block, preferred_element_type=jnp.float32
            )
            return (new_max, new_sum, new_acc)

        touches = (doc_block[0] <= last_doc) & (doc_block[-1] >= first_doc)
        return lax.cond(touches, absorb, lambda current: current, state)

    initial = (
        jnp.full((total_rows,), NEG, jnp.float32),
        jnp.zeros((total_rows,), jnp.float32),
        jnp.zeros((total_rows, head_dim), jnp.float32),
    )
    carry = initial
    shards = n
    joined = 1
    while joined * 2 <= shards and shards % (joined * 2) == 0 and (joined * 2 * tok_rows <= 1024):
        joined = joined * 2
    blocks = shards // joined
    span_rows = joined * tok_rows
    key_blocks = kv_all[..., :head_dim].reshape(blocks, span_rows, head_dim)
    value_blocks = kv_all[..., head_dim:].reshape(blocks, span_rows, head_dim)
    doc_blocks = doc_all.reshape(blocks, span_rows)

    def visit(state, inputs):
        key_block, value_block, doc_block = inputs
        return (absorb_block(state, key_block, value_block, doc_block), None)

    carry, unused = lax.scan(visit, carry, (key_blocks, value_blocks, doc_blocks))
    attended = (carry[2] / carry[1][:, None]).astype(jnp.bfloat16)
    attended = (
        attended.reshape(local_heads, tok_rows, head_dim)
        .transpose(1, 0, 2)
        .reshape(tok_rows, local_heads * head_dim)
    )
    partial_value = jnp.dot(attended, out_weight, preferred_element_type=jnp.float32)
    normed, resid = mid_stage(nt, partial_value.astype(jnp.bfloat16), tokens_in, norm_gain)
    normed = normed.reshape(2 * tok_rows, -1)
    both = jnp.dot(normed, gate_up_all, preferred_element_type=jnp.float32)
    units = both.shape[1] // 2
    hidden = (jax.nn.silu(both[:, :units]) * both[:, units:]).astype(jnp.bfloat16)
    fed_part = jnp.dot(hidden, down_all, preferred_element_type=jnp.float32)
    out = last_stage(nt, fed_part.astype(jnp.bfloat16), resid)
    return out.reshape(tok_rows, -1)


def solution(mesh):
    return jax.shard_map(
        functools.partial(per_device, mesh.shape["sp"], mesh.shape["tp"]),
        mesh=mesh,
        in_specs=(
            P("sp", None),
            P("sp", "tp"),
            P("sp", "tp"),
            P("sp", "tp"),
            P("sp"),
            P(),
            P(),
            P("tp", None),
            P(),
            P("sp", "tp"),
            P("sp", "tp"),
            P("tp", "sp"),
        ),
        out_specs=P("sp", None),
        check_vma=False,
    )
```

```python
import functools

import jax
import jax.numpy as jnp
from jax import lax
from jax.experimental import pallas as pl
from jax.experimental.pallas import tpu as pltpu
from jax.sharding import PartitionSpec as P

GRID = 64


EPS = 1e-06
THETA = 10000.0
NEG = -1e30


def rotate_half(block, angle):
    half_dim = block.shape[-1] // 2
    cosine = jnp.cos(angle)[:, None, :]
    sine = jnp.sin(angle)[:, None, :]
    first = block[..., :half_dim]
    second = block[..., half_dim:]
    return jnp.concatenate(
        [first * cosine - second * sine, second * cosine + first * sine], axis=-1
    )


def normalized_rotated(values_in, gain, heads, lattice_row, lattice_column):
    full = values_in.astype(jnp.float32).reshape(values_in.shape[0], heads, -1)
    full = full * lax.rsqrt(jnp.mean(full * full, axis=-1, keepdims=True) + EPS) * gain
    half_dim = full.shape[-1] // 2
    freqs = THETA ** (-2.0 * jnp.arange(half_dim // 2, dtype=jnp.float32) / half_dim)
    by_row = rotate_half(full[..., :half_dim], lattice_row[:, None] * freqs[None, :])
    by_col = rotate_half(full[..., half_dim:], lattice_column[:, None] * freqs[None, :])
    return jnp.concatenate([by_row, by_col], axis=-1).astype(jnp.bfloat16)


MESH = pl.DeviceIdType.MESH
VM = pl.BlockSpec(memory_space=pltpu.VMEM)


def params(cid):
    return pltpu.CompilerParams(
        collective_id=cid, has_side_effects=True, vmem_limit_bytes=56 * 1024 * 1024
    )


def greet(count, where):
    barrier = pltpu.get_barrier_semaphore()

    @pl.loop(1, count)
    def _(step):
        pl.semaphore_signal(barrier, inc=1, device_id=where(step), device_id_type=MESH)

    pl.semaphore_wait(barrier, count - 1)


def gather_kernel(n, kv_ref, doc_ref, kv_out, doc_out, send, recv, doc_send, doc_recv):
    me = lax.axis_index("sp")

    def where(step):
        return {"sp": lax.rem(me + step, n)}

    def copies(step, slot):
        return (
            pltpu.make_async_remote_copy(
                kv_ref, kv_out.at[slot], send.at[step], recv.at[step], where(step), MESH
            ),
            pltpu.make_async_remote_copy(
                doc_ref, doc_out.at[slot], doc_send.at[step], doc_recv.at[step], where(step), MESH
            ),
        )

    greet(n, where)

    @pl.loop(1, n)
    def _(step):
        for copy in copies(step, me):
            copy.start()

    kv_out[me] = kv_ref[...]
    doc_out[me] = doc_ref[...]

    @pl.loop(1, n)
    def _(step):
        for copy in copies(step, lax.rem(me + n - step, n)):
            copy.wait_recv()
            copy.wait_send()


def gather_sp(n, packed, docs):
    return pl.pallas_call(
        functools.partial(gather_kernel, n),
        out_shape=(
            jax.ShapeDtypeStruct((n,) + packed.shape, packed.dtype),
            jax.ShapeDtypeStruct((n,) + docs.shape, docs.dtype),
        ),
        in_specs=[VM, VM],
        out_specs=(VM, VM),
        scratch_shapes=[pltpu.SemaphoreType.DMA((n,))] * 4,
        compiler_params=params(0),
        name="gather_sp",
    )(packed, docs)


def mid_kernel(
    nt, partial_ref, tokens_ref, gain_ref, normed_out, resid_out, landing, send, recv, send2, recv2
):
    sp, tp = lax.axis_index("sp"), lax.axis_index("tp")
    side = lax.rem(sp, 2)
    base = sp - side
    group = 2 * nt
    me = side * nt + tp
    rows = resid_out.shape[0]

    def where(step):
        other = lax.rem(me + step, group)
        return {"sp": base + other // nt, "tp": lax.rem(other, nt)}

    def part(step):
        peer = lax.rem(tp + step, nt)
        return pltpu.make_async_remote_copy(
            partial_ref.at[peer],
            landing.at[step],
            send.at[step],
            recv.at[step],
            {"sp": sp, "tp": peer},
            MESH,
        )

    def spread(step, slot):
        return pltpu.make_async_remote_copy(
            normed_out.at[slot], normed_out.at[slot], send2.at[step], recv2.at[step], where(step), MESH
        )

    greet(group, where)
    for step in range(1, nt):
        part(step).start()
    for step in range(1, nt):
        part(step).wait_recv()
    chunk = 16

    @pl.loop(0, rows // chunk)
    def _(i):
        at = pl.ds(pl.multiple_of(i * chunk, chunk), chunk)
        mixed = partial_ref[tp, at].astype(jnp.float32)
        for step in range(1, nt):
            mixed = mixed + landing[step, at].astype(jnp.float32)
        resid = tokens_ref[tp, at].astype(jnp.float32) + mixed
        resid_out[at] = resid
        power = jnp.mean(resid * resid, axis=-1, keepdims=True)
        normed_out[me, at] = (resid * lax.rsqrt(power + EPS) * gain_ref[...]).astype(jnp.bfloat16)

    for step in range(1, group):
        spread(step, me).start()
    for step in range(1, group):
        copy = spread(step, lax.rem(me + group - step, group))
        copy.wait_recv()
        copy.wait_send()
    for step in range(1, nt):
        part(step).wait_send()


def mid_stage(nt, part, tokens, gain):
    rows, width = part.shape[0] // nt, part.shape[1]
    return pl.pallas_call(
        functools.partial(mid_kernel, nt),
        out_shape=(
            jax.ShapeDtypeStruct((2 * nt, rows, width), jnp.bfloat16),
            jax.ShapeDtypeStruct((rows, width), jnp.float32),
        ),
        in_specs=[VM, VM, VM],
        out_specs=(VM, VM),
        scratch_shapes=[pltpu.VMEM((nt, rows, width), jnp.bfloat16)]
        + [pltpu.SemaphoreType.DMA((nt,))] * 2
        + [pltpu.SemaphoreType.DMA((2 * nt,))] * 2,
        compiler_params=params(1),
        name="mid_stage",
    )(part.reshape(nt, rows, width), tokens.reshape(nt, rows, width), gain.reshape(1, width))


def last_kernel(nt, fed_ref, resid_ref, out_ref, landing, send, recv, send2, recv2):
    sp, tp = lax.axis_index("sp"), lax.axis_index("tp")
    side = lax.rem(sp, 2)
    base = sp - side
    group = 2 * nt
    me = side * nt + tp
    rows = resid_ref.shape[0]

    def where(step):
        other = lax.rem(me + step, group)
        return {"sp": base + other // nt, "tp": lax.rem(other, nt)}

    def part(step):
        return pltpu.make_async_remote_copy(
            fed_ref.at[lax.rem(me + step, group)],
            landing.at[step],
            send.at[step],
            recv.at[step],
            where(step),
            MESH,
        )

    def spread(step, slot):
        return pltpu.make_async_remote_copy(
            out_ref.at[slot],
            out_ref.at[slot],
            send2.at[step],
            recv2.at[step],
            {"sp": sp, "tp": lax.rem(tp + step, nt)},
            MESH,
        )

    greet(group, where)
    for step in range(1, group):
        part(step).start()
    for step in range(1, group):
        part(step).wait_recv()
    chunk = 16

    @pl.loop(0, rows // chunk)
    def _(i):
        at = pl.ds(pl.multiple_of(i * chunk, chunk), chunk)
        fed = fed_ref[me, at].astype(jnp.float32)
        for step in range(1, group):
            fed = fed + landing[step, at].astype(jnp.float32)
        out_ref[tp, at] = (resid_ref[at] + fed).astype(jnp.bfloat16)

    for step in range(1, nt):
        spread(step, tp).start()
    for step in range(1, nt):
        copy = spread(step, lax.rem(tp + nt - step, nt))
        copy.wait_recv()
        copy.wait_send()
    for step in range(1, group):
        part(step).wait_send()


def last_stage(nt, fed, resid):
    rows, width = resid.shape
    return pl.pallas_call(
        functools.partial(last_kernel, nt),
        out_shape=jax.ShapeDtypeStruct((nt, rows, width), jnp.bfloat16),
        in_specs=[VM, VM],
        out_specs=VM,
        scratch_shapes=[pltpu.VMEM((2 * nt, rows, width), jnp.bfloat16)]
        + [pltpu.SemaphoreType.DMA((2 * nt,))] * 2
        + [pltpu.SemaphoreType.DMA((nt,))] * 2,
        compiler_params=params(2),
        name="last_stage",
    )(fed.reshape(2 * nt, rows, width), resid)


def pair_share(n, arrays, axis, joins):
    side = lax.rem(lax.axis_index("sp"), 2)
    own, away = [], []
    for array in arrays:
        half = array.shape[axis] // 2
        own.append(lax.dynamic_slice_in_dim(array, side * half, half, axis))
        away.append(lax.dynamic_slice_in_dim(array, (1 - side) * half, half, axis))
    own = jnp.concatenate(own, axis=axis)
    away = jnp.concatenate(away, axis=axis)
    came = lax.ppermute(away, "sp", [(i, i ^ 1) for i in range(n)])
    first = jnp.where(side == 0, own, came)
    second = jnp.where(side == 0, came, own)
    return jnp.concatenate([first, second], axis=joins)


def per_device(
    n,
    nt,
    tokens_in,
    queries,
    keys,
    values,
    doc_ids,
    query_gain,
    key_norm_scale,
    out_weight,
    norm_gain,
    gate_weight,
    up_weight,
    down_weight,
):
    tok_rows = tokens_in.shape[0]
    head_dim = query_gain.shape[0]
    local_heads = queries.shape[1] // head_dim
    places = lax.axis_index("sp") * tok_rows + jnp.arange(tok_rows, dtype=jnp.int32)
    lattice_row = (places // GRID).astype(jnp.float32)
    lattice_column = (places % GRID).astype(jnp.float32)
    q_local = normalized_rotated(queries, query_gain, local_heads, lattice_row, lattice_column)
    q_rows = q_local.transpose(1, 0, 2).reshape(local_heads * tok_rows, head_dim)
    lanes = [[2 * j + side for j in range(n // 2)] for side in range(2)]
    gate_up_all = lax.all_gather(
        pair_share(n, [gate_weight, up_weight], 1, 0), "sp", axis_index_groups=lanes, axis=0, tiled=True
    )
    down_pair = pair_share(n, [down_weight], 0, 1)
    lane, count = lax.axis_index("sp") // 2, n // 2
    span = down_pair.shape[1]
    down_all = jnp.zeros((down_pair.shape[0], count * span), down_pair.dtype)
    for shift in range(count):
        piece = down_pair
        if shift:
            piece = lax.ppermute(down_pair, "sp", [(i, (i + 2 * shift) % n) for i in range(n)])
        down_all = lax.dynamic_update_slice_in_dim(
            down_all, piece, lax.rem(lane + count - shift, count) * span, 1
        )
    turned = normalized_rotated(keys, key_norm_scale, 1, lattice_row, lattice_column)
    packed = jnp.concatenate([turned.reshape(tok_rows, head_dim), values], axis=1)
    kv_all, doc_all = gather_sp(n, packed, doc_ids.reshape(1, tok_rows))
    row_docs = jnp.tile(doc_ids, local_heads)
    first_doc = doc_ids[0]
    last_doc = doc_ids[-1]
    scale = head_dim ** (-0.5)
    total_rows = local_heads * tok_rows

    def absorb_block(state, key_block, value_block, doc_block):

        def absorb(current):
            running_max, running_sum, running_acc = current
            scores = (
                jnp.einsum("qd,kd->qk", q_rows, key_block, preferred_element_type=jnp.float32)
                * scale
            )
            same = row_docs[:, None] == doc_block[None, :]
            scores = jnp.where(same, scores, NEG)
            new_max = jnp.maximum(running_max, jnp.max(scores, axis=1))
            weights = jnp.where(same, jnp.exp(scores - new_max[:, None]), 0.0)
            shrink = jnp.exp(running_max - new_max)
            new_sum = running_sum * shrink + jnp.sum(weights, axis=1)
            new_acc = running_acc * shrink[:, None] + jnp.dot(
                weights.astype(jnp.bfloat16), value_block, preferred_element_type=jnp.float32
            )
            return (new_max, new_sum, new_acc)

        touches = (doc_block[0] <= last_doc) & (doc_block[-1] >= first_doc)
        return lax.cond(touches, absorb, lambda current: current, state)

    initial = (
        jnp.full((total_rows,), NEG, jnp.float32),
        jnp.zeros((total_rows,), jnp.float32),
        jnp.zeros((total_rows, head_dim), jnp.float32),
    )
    carry = initial
    shards = n
    joined = 1
    while joined * 2 <= shards and shards % (joined * 2) == 0 and (joined * 2 * tok_rows <= 1024):
        joined = joined * 2
    blocks = shards // joined
    span_rows = joined * tok_rows
    key_blocks = kv_all[..., :head_dim].reshape(blocks, span_rows, head_dim)
    value_blocks = kv_all[..., head_dim:].reshape(blocks, span_rows, head_dim)
    doc_blocks = doc_all.reshape(blocks, span_rows)

    def visit(state, inputs):
        key_block, value_block, doc_block = inputs
        return (absorb_block(state, key_block, value_block, doc_block), None)

    carry, unused = lax.scan(visit, carry, (key_blocks, value_blocks, doc_blocks))
    attended = (carry[2] / carry[1][:, None]).astype(jnp.bfloat16)
    attended = (
        attended.reshape(local_heads, tok_rows, head_dim)
        .transpose(1, 0, 2)
        .reshape(tok_rows, local_heads * head_dim)
    )
    partial_value = jnp.dot(attended, out_weight, preferred_element_type=jnp.float32)
    normed, resid = mid_stage(nt, partial_value.astype(jnp.bfloat16), tokens_in, norm_gain)
    normed = normed.reshape(2 * tok_rows, -1)
    both = jnp.dot(normed, gate_up_all, preferred_element_type=jnp.float32)
    units = both.shape[1] // 2
    hidden = (jax.nn.silu(both[:, :units]) * both[:, units:]).astype(jnp.bfloat16)
    fed_part = jnp.dot(hidden, down_all, preferred_element_type=jnp.float32)
    out = last_stage(nt, fed_part.astype(jnp.bfloat16), resid)
    return out.reshape(tok_rows, -1)


def solution(mesh):
    return jax.shard_map(
        functools.partial(per_device, mesh.shape["sp"], mesh.shape["tp"]),
        mesh=mesh,
        in_specs=(
            P("sp", None),
            P("sp", "tp"),
            P("sp", "tp"),
            P("sp", "tp"),
            P("sp"),
            P(),
            P(),
            P("tp", None),
            P(),
            P("sp", "tp"),
            P("sp", "tp"),
            P("tp", "sp"),
        ),
        out_specs=P("sp", None),
        check_vma=False,
    )
```

```python
import functools

import jax
import jax.numpy as jnp
from jax import lax
from jax.experimental import pallas as pl
from jax.experimental.pallas import tpu as pltpu
from jax.sharding import PartitionSpec as P

GRID = 64


EPS = 1e-06
THETA = 10000.0
NEG = -1e30


def rotate_half(block, angle):
    half_dim = block.shape[-1] // 2
    cosine = jnp.cos(angle)[:, None, :]
    sine = jnp.sin(angle)[:, None, :]
    first = block[..., :half_dim]
    second = block[..., half_dim:]
    return jnp.concatenate(
        [first * cosine - second * sine, second * cosine + first * sine], axis=-1
    )


def normalized_rotated(values_in, gain, heads, lattice_row, lattice_column):
    full = values_in.astype(jnp.float32).reshape(values_in.shape[0], heads, -1)
    full = full * lax.rsqrt(jnp.mean(full * full, axis=-1, keepdims=True) + EPS) * gain
    half_dim = full.shape[-1] // 2
    freqs = THETA ** (-2.0 * jnp.arange(half_dim // 2, dtype=jnp.float32) / half_dim)
    by_row = rotate_half(full[..., :half_dim], lattice_row[:, None] * freqs[None, :])
    by_col = rotate_half(full[..., half_dim:], lattice_column[:, None] * freqs[None, :])
    return jnp.concatenate([by_row, by_col], axis=-1).astype(jnp.bfloat16)


MESH = pl.DeviceIdType.MESH
VM = pl.BlockSpec(memory_space=pltpu.VMEM)


def params(cid):
    return pltpu.CompilerParams(
        collective_id=cid, has_side_effects=True, vmem_limit_bytes=56 * 1024 * 1024
    )


def greet(count, where):
    barrier = pltpu.get_barrier_semaphore()

    @pl.loop(1, count)
    def _(step):
        pl.semaphore_signal(barrier, inc=1, device_id=where(step), device_id_type=MESH)

    pl.semaphore_wait(barrier, count - 1)


def gather_kernel(n, kv_ref, doc_ref, kv_out, doc_out, send, recv, doc_send, doc_recv):
    me = lax.axis_index("sp")

    def where(step):
        return {"sp": lax.rem(me + step, n)}

    def copies(step, slot):
        return (
            pltpu.make_async_remote_copy(
                kv_ref, kv_out.at[slot], send.at[step], recv.at[step], where(step), MESH
            ),
            pltpu.make_async_remote_copy(
                doc_ref, doc_out.at[slot], doc_send.at[step], doc_recv.at[step], where(step), MESH
            ),
        )

    greet(n, where)

    @pl.loop(1, n)
    def _(step):
        for copy in copies(step, me):
            copy.start()

    kv_out[me] = kv_ref[...]
    doc_out[me] = doc_ref[...]

    @pl.loop(1, n)
    def _(step):
        for copy in copies(step, lax.rem(me + n - step, n)):
            copy.wait_recv()
            copy.wait_send()


def gather_sp(n, packed, docs):
    return pl.pallas_call(
        functools.partial(gather_kernel, n),
        out_shape=(
            jax.ShapeDtypeStruct((n,) + packed.shape, packed.dtype),
            jax.ShapeDtypeStruct((n,) + docs.shape, docs.dtype),
        ),
        in_specs=[VM, VM],
        out_specs=(VM, VM),
        scratch_shapes=[pltpu.SemaphoreType.DMA((n,))] * 4,
        compiler_params=params(0),
        name="gather_sp",
    )(packed, docs)


def mid_kernel(
    nt, partial_ref, tokens_ref, gain_ref, normed_out, resid_out, landing, send, recv, send2, recv2
):
    sp, tp = lax.axis_index("sp"), lax.axis_index("tp")
    side = lax.rem(sp, 2)
    base = sp - side
    group = 2 * nt
    me = side * nt + tp
    rows = resid_out.shape[0]

    def where(step):
        other = lax.rem(me + step, group)
        return {"sp": base + other // nt, "tp": lax.rem(other, nt)}

    def part(step):
        peer = lax.rem(tp + step, nt)
        return pltpu.make_async_remote_copy(
            partial_ref.at[peer],
            landing.at[step],
            send.at[step],
            recv.at[step],
            {"sp": sp, "tp": peer},
            MESH,
        )

    def spread(step, slot):
        return pltpu.make_async_remote_copy(
            normed_out.at[slot], normed_out.at[slot], send2.at[step], recv2.at[step], where(step), MESH
        )

    greet(group, where)
    for step in range(1, nt):
        part(step).start()
    for step in range(1, nt):
        part(step).wait_recv()
    chunk = 16

    @pl.loop(0, rows // chunk)
    def _(i):
        at = pl.ds(pl.multiple_of(i * chunk, chunk), chunk)
        mixed = partial_ref[tp, at].astype(jnp.float32)
        for step in range(1, nt):
            mixed = mixed + landing[step, at].astype(jnp.float32)
        resid = tokens_ref[tp, at].astype(jnp.float32) + mixed
        resid_out[at] = resid
        power = jnp.mean(resid * resid, axis=-1, keepdims=True)
        normed_out[me, at] = (resid * lax.rsqrt(power + EPS) * gain_ref[...]).astype(jnp.bfloat16)

    for step in range(1, group):
        spread(step, me).start()
    for step in range(1, group):
        copy = spread(step, lax.rem(me + group - step, group))
        copy.wait_recv()
        copy.wait_send()
    for step in range(1, nt):
        part(step).wait_send()


def mid_stage(nt, part, tokens, gain):
    rows, width = part.shape[0] // nt, part.shape[1]
    return pl.pallas_call(
        functools.partial(mid_kernel, nt),
        out_shape=(
            jax.ShapeDtypeStruct((2 * nt, rows, width), jnp.bfloat16),
            jax.ShapeDtypeStruct((rows, width), jnp.float32),
        ),
        in_specs=[VM, VM, VM],
        out_specs=(VM, VM),
        scratch_shapes=[pltpu.VMEM((nt, rows, width), jnp.bfloat16)]
        + [pltpu.SemaphoreType.DMA((nt,))] * 2
        + [pltpu.SemaphoreType.DMA((2 * nt,))] * 2,
        compiler_params=params(1),
        name="mid_stage",
    )(part.reshape(nt, rows, width), tokens.reshape(nt, rows, width), gain.reshape(1, width))


def last_kernel(nt, fed_ref, resid_ref, out_ref, landing, send, recv, send2, recv2):
    sp, tp = lax.axis_index("sp"), lax.axis_index("tp")
    side = lax.rem(sp, 2)
    base = sp - side
    group = 2 * nt
    me = side * nt + tp
    rows = resid_ref.shape[0]

    def where(step):
        other = lax.rem(me + step, group)
        return {"sp": base + other // nt, "tp": lax.rem(other, nt)}

    def part(step):
        return pltpu.make_async_remote_copy(
            fed_ref.at[lax.rem(me + step, group)],
            landing.at[step],
            send.at[step],
            recv.at[step],
            where(step),
            MESH,
        )

    def spread(step, slot):
        return pltpu.make_async_remote_copy(
            out_ref.at[slot],
            out_ref.at[slot],
            send2.at[step],
            recv2.at[step],
            {"sp": sp, "tp": lax.rem(tp + step, nt)},
            MESH,
        )

    greet(group, where)
    for step in range(1, group):
        part(step).start()
    for step in range(1, group):
        part(step).wait_recv()
    chunk = 16

    @pl.loop(0, rows // chunk)
    def _(i):
        at = pl.ds(pl.multiple_of(i * chunk, chunk), chunk)
        fed = fed_ref[me, at].astype(jnp.float32)
        for step in range(1, group):
            fed = fed + landing[step, at].astype(jnp.float32)
        out_ref[tp, at] = (resid_ref[at] + fed).astype(jnp.bfloat16)

    for step in range(1, nt):
        spread(step, tp).start()
    for step in range(1, nt):
        copy = spread(step, lax.rem(tp + nt - step, nt))
        copy.wait_recv()
        copy.wait_send()
    for step in range(1, group):
        part(step).wait_send()


def last_stage(nt, fed, resid):
    rows, width = resid.shape
    return pl.pallas_call(
        functools.partial(last_kernel, nt),
        out_shape=jax.ShapeDtypeStruct((nt, rows, width), jnp.bfloat16),
        in_specs=[VM, VM],
        out_specs=VM,
        scratch_shapes=[pltpu.VMEM((2 * nt, rows, width), jnp.bfloat16)]
        + [pltpu.SemaphoreType.DMA((2 * nt,))] * 2
        + [pltpu.SemaphoreType.DMA((nt,))] * 2,
        compiler_params=params(2),
        name="last_stage",
    )(fed.reshape(2 * nt, rows, width), resid)


def pair_share(n, arrays, axis, joins):
    side = lax.rem(lax.axis_index("sp"), 2)
    own, away = [], []
    for array in arrays:
        half = array.shape[axis] // 2
        own.append(lax.dynamic_slice_in_dim(array, side * half, half, axis))
        away.append(lax.dynamic_slice_in_dim(array, (1 - side) * half, half, axis))
    own = jnp.concatenate(own, axis=axis)
    away = jnp.concatenate(away, axis=axis)
    came = lax.ppermute(away, "sp", [(i, i ^ 1) for i in range(n)])
    first = jnp.where(side == 0, own, came)
    second = jnp.where(side == 0, came, own)
    return jnp.concatenate([first, second], axis=joins)


def per_device(
    n,
    nt,
    tokens_in,
    queries,
    keys,
    values,
    doc_ids,
    query_gain,
    key_norm_scale,
    out_weight,
    norm_gain,
    gate_weight,
    up_weight,
    down_weight,
):
    tok_rows = tokens_in.shape[0]
    head_dim = query_gain.shape[0]
    local_heads = queries.shape[1] // head_dim
    places = lax.axis_index("sp") * tok_rows + jnp.arange(tok_rows, dtype=jnp.int32)
    lattice_row = (places // GRID).astype(jnp.float32)
    lattice_column = (places % GRID).astype(jnp.float32)
    q_local = normalized_rotated(queries, query_gain, local_heads, lattice_row, lattice_column)
    q_rows = q_local.transpose(1, 0, 2).reshape(local_heads * tok_rows, head_dim)
    lanes = [[2 * j + side for j in range(n // 2)] for side in range(2)]
    down_pair = pair_share(n, [down_weight], 0, 1)
    down_pair, gate_own, up_own = lax.optimization_barrier((down_pair, gate_weight, up_weight))
    down_all = lax.all_gather(down_pair, "sp", axis_index_groups=lanes, axis=1, tiled=True)
    gate_up_all = lax.all_gather(
        pair_share(n, [gate_own, up_own], 1, 0), "sp", axis_index_groups=lanes, axis=0, tiled=True
    )
    turned = normalized_rotated(keys, key_norm_scale, 1, lattice_row, lattice_column)
    packed = jnp.concatenate([turned.reshape(tok_rows, head_dim), values], axis=1)
    kv_all, doc_all = gather_sp(n, packed, doc_ids.reshape(1, tok_rows))
    row_docs = jnp.tile(doc_ids, local_heads)
    first_doc = doc_ids[0]
    last_doc = doc_ids[-1]
    scale = head_dim ** (-0.5)
    total_rows = local_heads * tok_rows

    def absorb_block(state, key_block, value_block, doc_block):

        def absorb(current):
            running_max, running_sum, running_acc = current
            scores = (
                jnp.einsum("qd,kd->qk", q_rows, key_block, preferred_element_type=jnp.float32)
                * scale
            )
            same = row_docs[:, None] == doc_block[None, :]
            scores = jnp.where(same, scores, NEG)
            new_max = jnp.maximum(running_max, jnp.max(scores, axis=1))
            weights = jnp.where(same, jnp.exp(scores - new_max[:, None]), 0.0)
            shrink = jnp.exp(running_max - new_max)
            new_sum = running_sum * shrink + jnp.sum(weights, axis=1)
            new_acc = running_acc * shrink[:, None] + jnp.dot(
                weights.astype(jnp.bfloat16), value_block, preferred_element_type=jnp.float32
            )
            return (new_max, new_sum, new_acc)

        touches = (doc_block[0] <= last_doc) & (doc_block[-1] >= first_doc)
        return lax.cond(touches, absorb, lambda current: current, state)

    initial = (
        jnp.full((total_rows,), NEG, jnp.float32),
        jnp.zeros((total_rows,), jnp.float32),
        jnp.zeros((total_rows, head_dim), jnp.float32),
    )
    carry = initial
    shards = n
    joined = 1
    while joined * 2 <= shards and shards % (joined * 2) == 0 and (joined * 2 * tok_rows <= 1024):
        joined = joined * 2
    blocks = shards // joined
    span_rows = joined * tok_rows
    key_blocks = kv_all[..., :head_dim].reshape(blocks, span_rows, head_dim)
    value_blocks = kv_all[..., head_dim:].reshape(blocks, span_rows, head_dim)
    doc_blocks = doc_all.reshape(blocks, span_rows)

    def visit(state, inputs):
        key_block, value_block, doc_block = inputs
        return (absorb_block(state, key_block, value_block, doc_block), None)

    carry, unused = lax.scan(visit, carry, (key_blocks, value_blocks, doc_blocks))
    attended = (carry[2] / carry[1][:, None]).astype(jnp.bfloat16)
    attended = (
        attended.reshape(local_heads, tok_rows, head_dim)
        .transpose(1, 0, 2)
        .reshape(tok_rows, local_heads * head_dim)
    )
    partial_value = jnp.dot(attended, out_weight, preferred_element_type=jnp.float32)
    normed, resid = mid_stage(nt, partial_value.astype(jnp.bfloat16), tokens_in, norm_gain)
    normed = normed.reshape(2 * tok_rows, -1)
    both = jnp.dot(normed, gate_up_all, preferred_element_type=jnp.float32)
    units = both.shape[1] // 2
    hidden = (jax.nn.silu(both[:, :units]) * both[:, units:]).astype(jnp.bfloat16)
    fed_part = jnp.dot(hidden, down_all, preferred_element_type=jnp.float32)
    out = last_stage(nt, fed_part.astype(jnp.bfloat16), resid)
    return out.reshape(tok_rows, -1)


def solution(mesh):
    return jax.shard_map(
        functools.partial(per_device, mesh.shape["sp"], mesh.shape["tp"]),
        mesh=mesh,
        in_specs=(
            P("sp", None),
            P("sp", "tp"),
            P("sp", "tp"),
            P("sp", "tp"),
            P("sp"),
            P(),
            P(),
            P("tp", None),
            P(),
            P("sp", "tp"),
            P("sp", "tp"),
            P("tp", "sp"),
        ),
        out_specs=P("sp", None),
        check_vma=False,
    )
```
